32 devices in a mesh: sp: 8 (over z, x), tp: 4 (over y, core).
Axes of the slice: x: 2, y: 2, z: 4, core: 2. Of those that a mesh axis runs over, the one named last changes fastest.
Arguments:
- stream: bfloat16 [1024, 2048], P(('sp', 'tp')), may hold values from -2.5 to 2.5
- recurrence_input: bfloat16 [1024, 2, 1024], P('sp', None, 'tp'), may hold values from -6 to 6
- output_gate_input: bfloat16 [1024, 2, 1024], P('sp', None, 'tp'), may hold values from -6 to 6
- convolution_taps: bfloat16 [4, 2, 1024], P(None, None, 'tp'), may hold values from -4 to 4
- first_group_gates: bfloat16 [2, 16, 64, 64], P(None, 'tp'), may hold values from -0.75 to 0.75
- second_group_gates: bfloat16 [2, 8, 128, 128], P(None, 'tp'), may hold values from -0.5 to 0.5
- channel_decay: float32 [2, 1024], P(None, 'tp'), may hold values from 4.7 to 13.6
- position_log_extra: float32 [1024, 2, 1024], P('sp', None, 'tp'), may hold values from -1.4 to 0, as said below
- recurrence_output_weight: bfloat16 [2, 1024, 2048], P(None, 'tp'), may hold values from -0.125 to 0.125
- first_norm_gain: float32 [2048], replicated, may hold values from 0.1 to 1.9
- first_norm_bias: float32 [2048], replicated, may hold values from -1.75 to 1.75
- routed_expert_index: int32 [1024, 4], P('sp'), may hold values from 0 to 7, all different within a row; in each aligned block of 32 rows (0 to 31, 32 to 63, ...) at most 20 rows name the same one
- routed_expert_weight: float32 [1024, 4], P('sp'), may hold values from 0.25 to 1
- routed_gate_weight: bfloat16 [8, 2048, 512], P('sp', None, 'tp'), may hold values from -0.125 to 0.125
- routed_up_weight: bfloat16 [8, 2048, 512], P('sp', None, 'tp'), may hold values from -0.125 to 0.125
- routed_down_weight: bfloat16 [8, 512, 2048], P('sp', 'tp'), may hold values from -0.25 to 0.25
- shared_gate_weight: bfloat16 [2048, 512], replicated, may hold values from -0.125 to 0.125
- shared_up_weight: bfloat16 [2048, 512], replicated, may hold values from -0.125 to 0.125
- shared_down_weight: bfloat16 [512, 2048], replicated, may hold values from -0.25 to 0.25
- second_norm_gain: float32 [2048], replicated, may hold values from 0.1 to 1.9
- second_norm_bias: float32 [2048], replicated, may hold values from -1.75 to 1.75
Outputs:
- result: bfloat16 [1024, 2048], P(('sp', 'tp'))
The draws below stay inside these ranges and needn't reach their ends.
Inputs may be any that keep to these rules, and one draw needn't show every extreme that they name: `routed_expert_index`: each row names 4 different experts. In each aligned block of 32 rows no expert is named more than 20 times, and in some block an expert is named exactly 20 times. `position_log_extra`: every entry is negative.
All inputs are finite; a program needn't handle non-finite values.
Results may differ from the reference program's by a relative error of at most 0.015.
Values may be sent and summed in bfloat16 or wider, within the bound.
A program may use at most 64 MiB of HBM per device.

```python
import math
import jax
import jax.numpy as jnp
import numpy as np
from jax import lax

D = 2048
D_HALF = 1024
HEAD_SMALL = 64
HEAD_LARGE = 128
HEADS_SMALL = 16
HEADS_LARGE = 8
DQ = 256
CONV = 4
FE = 512
FE_DEV = 128
FS = 512
K = 4
EXPERTS = 8
TOK_DEV = 128
TOK_Q = 32
TOKENS = 1024
CAP_Q = 20
N_TP = 4


def draw_channel_decay(key, part):
    key_flag = jax.random.fold_in(key, 11)
    key_rate = jax.random.fold_in(key, 12)
    fast_limit = 5
    flags = jax.random.randint(key_flag, (2, D_HALF // HEAD_SMALL), 0, 10) < fast_limit
    channel = jnp.arange(D_HALF)
    head_index = jnp.stack([channel // HEAD_SMALL, channel // HEAD_LARGE])
    fast = jnp.take_along_axis(flags, head_index, axis=1)
    spread = jax.random.uniform(key_rate, (2, D_HALF), jnp.float32)
    fast_rate = jnp.exp(jnp.log(0.005) + spread * jnp.log(0.009 / 0.005))
    slow_rate = jnp.exp(jnp.log(1.25e-06) + spread * jnp.log(4.0))
    rate = jnp.where(fast, fast_rate, slow_rate)
    return -jnp.log(jnp.expm1(rate))


def draw_position_log_extra(key, part):
    key_base = jax.random.fold_in(key, 21)
    key_spot = jax.random.fold_in(key, 22)
    key_depth = jax.random.fold_in(key, 23)
    block_count = TOKENS // TOK_DEV
    base = jnp.exp(jax.random.uniform(key_base, (block_count, 1, 2, D_HALF), jnp.float32, jnp.log(5e-06), jnp.log(2e-05)))
    base = jnp.broadcast_to(base, (block_count, TOK_DEV, 2, D_HALF)).reshape(TOKENS, 2, D_HALF)
    spots = jax.random.randint(key_spot, (2,), 0, TOKENS)
    position = jnp.arange(TOKENS)
    hits = jnp.sum((position[:, None] == spots[None, :]).astype(jnp.float32), axis=1)
    depth = jax.random.uniform(key_depth, (2, D_HALF), jnp.float32, 0.22, 0.69)
    return -(base + hits[:, None, None] * depth[None])


def levels(own_key, shape, split, low, top_value):
    level, own = 1.0, jax.random.fold_in(own_key, 6)
    for dim, parts in split:
        heights = jnp.exp(jax.random.uniform(jax.random.fold_in(own, dim), (parts,), jnp.float32, low / len(split), top_value / len(split)))
        level = level * jnp.repeat(heights, shape[dim] // parts).reshape([-1 if axis == dim else 1 for axis in range(len(shape))])
    return level


def deal_out(rng, own, number, rows, count, top, limit, slope):
    sequence = jax.random.permutation(rng, count)
    heavy_load, ordinary = portions_of(count, rows * top, limit, slope, True), portions_of(count, rows * top, limit, slope, False)
    places = jnp.arange(count)

    def named(tallies, rotation):
        used = int((tallies > 0).sum())
        fixed = max(1, used // 4)
        moved = fixed + (places - fixed + rotation * (used - fixed)) % max(1, count - fixed)
        return jnp.zeros((count,), jnp.int32).at[sequence[jnp.where(places < fixed, places, moved)]].set(jnp.asarray(tallies, jnp.int32))

    tallies = jnp.where(number % 4 == 0, named(heavy_load, number // 4), named(ordinary, number - number // 4 - 1))
    mixed = jax.random.permutation(jax.random.fold_in(own, 3), count)
    donor, sink = mixed[0:count // 2 * 2:2], mixed[1:count // 2 * 2:2]
    margin = jnp.minimum(tallies[donor] - 1, limit - tallies[sink]) // 2
    margin = jnp.where((donor == sequence[0]) | (sink == sequence[0]) | (tallies[sink] == 0), 0, jnp.maximum(margin, 0))
    moved = jax.random.randint(jax.random.fold_in(own, 4), (count // 2,), 0, 1 << 20) % (margin + 1)
    tallies = tallies.at[donor].add(-moved).at[sink].add(moved)
    items = jnp.searchsorted(jnp.cumsum(tallies), jnp.arange(rows * top), side="right").astype(jnp.int32)
    table = items.reshape(top, rows).T
    table = table[jax.random.permutation(jax.random.fold_in(own, 1), rows)]
    rotation = jax.random.randint(jax.random.fold_in(own, 2), (rows, 1), 0, top)
    return jnp.take_along_axis(table, (jnp.arange(top)[None, :] + rotation) % top, axis=1)


def portions_of(number_of, total, reach, skew, full):
    portions = [(1 << 20) // math.isqrt(grade ** skew) + 1 for grade in range(1, number_of + 1)]
    largest = reach if full else min(reach, max(-(-total // number_of), total * portions[0] // sum(portions)))
    least = 1 if total - largest >= number_of - 1 else 0
    counts, spare = [largest] + [least] * (number_of - 1), total - largest - least * (number_of - 1)
    while spare > 0:
        movable = [i for i in range(1, number_of) if counts[i] < largest] or [i for i in range(1, number_of) if counts[i] < reach]
        mass, budget = sum([portions[i] for i in movable]), spare
        for i in movable:
            more = min(reach - counts[i], max(1, budget * portions[i] // mass), spare)
            counts[i] = counts[i] + more
            spare = spare - more
    return np.array(counts)


def noise(key, dims, scale, most, pieces=(), held_as=jnp.bfloat16):
    array = jax.random.normal(key, dims, jnp.float32) * scale
    if len(pieces) > 0:
        array = levels(key, dims, pieces, -0.22, 0.18) * array
    return jnp.clip(array, min=-most, max=most).astype(held_as)


def setup_inputs(seed: int = 0) -> dict:
    streams_of = jax.random.split(jax.random.key(seed), 22)
    stream = noise(streams_of[0], (TOKENS, D), 0.4, 2.5, ((0, 32),))
    recurrence_input = noise(streams_of[1], (TOKENS, 2, D_HALF), 1.0, 6.0, ((0, 8), (2, 4)))
    output_gate_input = noise(streams_of[2], (TOKENS, 2, D_HALF), 1.0, 6.0, ((0, 8), (2, 4)))
    convolution_taps = noise(streams_of[3], (CONV, 2, D_HALF), 1.0, 4.0, ((2, 4),))
    first_group_gates = noise(streams_of[4], (2, HEADS_SMALL, HEAD_SMALL, HEAD_SMALL), HEAD_SMALL ** -0.5, 0.75, ((1, 4),))
    second_group_gates = noise(streams_of[5], (2, HEADS_LARGE, HEAD_LARGE, HEAD_LARGE), HEAD_LARGE ** -0.5, 0.5, ((1, 4),))
    channel_decay = draw_channel_decay(jax.random.fold_in(streams_of[21], 71), 0)
    position_log_extra = draw_position_log_extra(jax.random.fold_in(streams_of[21], 71), 0)
    recurrence_output_weight = noise(streams_of[8], (2, D_HALF, D), (2 * D_HALF) ** -0.5, 0.125, ((1, 4),))
    first_norm_gain = jnp.clip(1.0 + 0.18 * jax.random.normal(streams_of[9], (D,), jnp.float32), 0.1, 1.9)
    first_norm_bias = noise(streams_of[10], (D,), 0.3, 1.75, (), jnp.float32)
    routed_expert_index_keys = jax.random.split(jax.random.fold_in(streams_of[11], 1), TOKENS // TOK_Q)
    routed_expert_index_turns = jax.random.permutation(jax.random.fold_in(streams_of[11], 3), TOKENS // TOK_Q)
    routed_expert_index = jax.vmap(lambda own, number: deal_out(jax.random.fold_in(streams_of[11], 2), own, number, TOK_Q, EXPERTS, K, CAP_Q, 1))(routed_expert_index_keys, routed_expert_index_turns).reshape((TOKENS, K))
    routed_expert_weight = jnp.clip(0.25 + 0.75 * jax.random.uniform(streams_of[12], (TOKENS, K), jnp.float32) ** levels(streams_of[12], (TOKENS, K), ((0, 8),), -0.2, 0.2), 0.25, 1.0)
    routed_gate_weight = noise(streams_of[13], (EXPERTS, D, FE), D ** -0.5, 0.125, ((0, 8), (2, 4)))
    routed_up_weight = noise(streams_of[14], (EXPERTS, D, FE), D ** -0.5, 0.125, ((0, 8), (2, 4)))
    routed_down_weight = noise(streams_of[15], (EXPERTS, FE, D), FE ** -0.5, 0.25, ((0, 8), (1, 4)))
    shared_gate_weight = noise(streams_of[16], (D, FS), D ** -0.5, 0.125)
    shared_up_weight = noise(streams_of[17], (D, FS), D ** -0.5, 0.125)
    shared_down_weight = noise(streams_of[18], (FS, D), FS ** -0.5, 0.25)
    second_norm_gain = jnp.clip(1.0 + 0.18 * jax.random.normal(streams_of[19], (D,), jnp.float32), 0.1, 1.9)
    second_norm_bias = noise(streams_of[20], (D,), 0.3, 1.75, (), jnp.float32)
    return {"stream": stream, "recurrence_input": recurrence_input, "output_gate_input": output_gate_input, "convolution_taps": convolution_taps, "first_group_gates": first_group_gates, "second_group_gates": second_group_gates, "channel_decay": channel_decay, "position_log_extra": position_log_extra, "recurrence_output_weight": recurrence_output_weight, "first_norm_gain": first_norm_gain, "first_norm_bias": first_norm_bias, "routed_expert_index": routed_expert_index, "routed_expert_weight": routed_expert_weight, "routed_gate_weight": routed_gate_weight, "routed_up_weight": routed_up_weight, "routed_down_weight": routed_down_weight, "shared_gate_weight": shared_gate_weight, "shared_up_weight": shared_up_weight, "shared_down_weight": shared_down_weight, "second_norm_gain": second_norm_gain, "second_norm_bias": second_norm_bias}


RESIDUAL_SCALE = 8.0 ** 0.25
NORM_EPSILON = 1e-05

def layer_norm(values, gain_vec, bias_vec):
    row_mean = lax.optimization_barrier(jnp.mean(values, axis=-1, keepdims=True))
    spread = lax.optimization_barrier(jnp.mean(jnp.square(values - row_mean), axis=-1, keepdims=True))
    return (values - row_mean) * lax.rsqrt(spread + NORM_EPSILON) * gain_vec + bias_vec

def rounded(values):
    return lax.optimization_barrier(values.astype(jnp.bfloat16)).astype(jnp.float32)

def block_gates(conv_rows, weights, head_size):
    length = conv_rows.shape[0]
    head_rows = conv_rows.reshape(length, -1, head_size).astype(jnp.float32)
    pre_act = jnp.einsum('thc,ghcd->gthd', head_rows, weights.astype(jnp.float32))
    gate_pair = jax.nn.sigmoid(pre_act).reshape(2, length, -1)
    return (gate_pair[0], gate_pair[1])

def chain_link(first_part, second_part):
    return (first_part[0] * second_part[0], second_part[0] * first_part[1] + second_part[1])

def recurrence_result(recurrence_input, output_gate_input, convolution_taps, first_group_gates, second_group_gates, channel_decay, position_log_extra):
    length = recurrence_input.shape[0]
    tap_count = convolution_taps.shape[0]
    padded = jnp.pad(recurrence_input.astype(jnp.float32), ((tap_count - 1, 0), (0, 0), (0, 0)))
    tap_weights = convolution_taps.astype(jnp.float32)
    summed = tap_weights[0] * padded[0:length]
    for offset in range(1, tap_count):
        summed = summed + tap_weights[offset] * padded[offset:offset + length]
    conv_rows = summed.astype(jnp.bfloat16)
    recur_a, input_a = block_gates(conv_rows[:, 0], first_group_gates, first_group_gates.shape[-1])
    recur_b, input_b = block_gates(conv_rows[:, 1], second_group_gates, second_group_gates.shape[-1])
    recurrence_gate = jnp.stack([recur_a, recur_b], axis=1)
    input_gate = jnp.stack([input_a, input_b], axis=1)
    decay_logarithm = -8.0 * recurrence_gate * jax.nn.softplus(-channel_decay) + position_log_extra
    driving = jnp.sqrt(-jnp.expm1(2.0 * decay_logarithm)) * input_gate * conv_rows.astype(jnp.float32)
    states = lax.associative_scan(chain_link, (jnp.exp(decay_logarithm), driving), axis=0)[1]
    return (jax.nn.gelu(output_gate_input.astype(jnp.float32)) * states).astype(jnp.bfloat16)

def reference(stream, recurrence_input, output_gate_input, convolution_taps, first_group_gates, second_group_gates, channel_decay, position_log_extra, recurrence_output_weight, first_norm_gain, first_norm_bias, routed_expert_index, routed_expert_weight, routed_gate_weight, routed_up_weight, routed_down_weight, shared_gate_weight, shared_up_weight, shared_down_weight, second_norm_gain, second_norm_bias):
    branch_output = recurrence_result(recurrence_input, output_gate_input, convolution_taps, first_group_gates, second_group_gates, channel_decay, position_log_extra)
    run_rows = branch_output.reshape(TOKENS, 2, N_TP, DQ)
    run_weights = recurrence_output_weight.reshape(2, N_TP, DQ, D)
    mixed = jnp.zeros((TOKENS, D), jnp.float32)
    for run_index in range(N_TP):
        partial_value = jnp.einsum('tgc,gcd->td', run_rows[:, :, run_index].astype(jnp.float32), run_weights[:, run_index].astype(jnp.float32))
        mixed = mixed + rounded(partial_value)
    normed = layer_norm(RESIDUAL_SCALE * stream.astype(jnp.float32) + mixed, first_norm_gain, first_norm_bias).astype(jnp.bfloat16)
    block_count = TOKENS // TOK_Q
    block_ids = routed_expert_index.reshape(block_count, TOK_Q * K)
    onehot = (block_ids[:, :, None] == jnp.arange(EXPERTS, dtype=jnp.int32)[None, None, :]).astype(jnp.int32)
    slot_ranks = lax.optimization_barrier(jnp.sum((jnp.cumsum(onehot, axis=1) - onehot) * onehot, axis=2)).astype(jnp.int32)
    targets = (block_ids * block_count + jnp.arange(block_count, dtype=jnp.int32)[:, None]) * CAP_Q + slot_ranks
    entries = jnp.arange(TOKENS * K, dtype=jnp.int32).reshape(block_count, TOK_Q * K)
    table = jnp.full((EXPERTS * block_count * CAP_Q,), TOKENS * K, jnp.int32)
    table = table.at[targets.reshape(-1)].set(entries.reshape(-1)).reshape(EXPERTS, block_count * CAP_Q)
    padded_rows = jnp.concatenate([normed, jnp.zeros((1, D), jnp.bfloat16)], axis=0)
    padded_weights = jnp.concatenate([routed_expert_weight.reshape(-1), jnp.zeros((1,), jnp.float32)])

    def expert_step(routed, inputs):
        entry_rows, gate_w, up_w, down_w = inputs
        token_rows = entry_rows // K
        picked = padded_rows[token_rows]
        hidden = (jax.nn.silu(jnp.dot(picked, gate_w, preferred_element_type=jnp.float32)) * jnp.dot(picked, up_w, preferred_element_type=jnp.float32)).astype(jnp.bfloat16)
        summed_out = jnp.zeros((picked.shape[0], D), jnp.float32)
        for run_index in range(N_TP):
            partial_out = jnp.dot(hidden[:, run_index * FE_DEV:(run_index + 1) * FE_DEV], down_w[run_index * FE_DEV:(run_index + 1) * FE_DEV], preferred_element_type=jnp.float32)
            summed_out = summed_out + rounded(partial_out)
        weighted = padded_weights[entry_rows][:, None] * rounded(summed_out)
        return (routed.at[token_rows].add(weighted), None)
    routed = lax.scan(expert_step, jnp.zeros((TOKENS + 1, D), jnp.float32), (table, routed_gate_weight, routed_up_weight, routed_down_weight))[0][:TOKENS]
    shared_hidden = (jax.nn.silu(jnp.dot(normed, shared_gate_weight, preferred_element_type=jnp.float32)) * jnp.dot(normed, shared_up_weight, preferred_element_type=jnp.float32)).astype(jnp.bfloat16)
    shared_out = jnp.dot(shared_hidden, shared_down_weight, preferred_element_type=jnp.float32)
    moe = shared_out + routed
    final = layer_norm(RESIDUAL_SCALE * normed.astype(jnp.float32) + moe, second_norm_gain, second_norm_bias)
    return final.astype(jnp.bfloat16)
```

```python
import functools

import jax
import jax.numpy as jnp
from jax import lax
from jax.experimental import pallas as pl
from jax.experimental.pallas import tpu as pltpu
from jax.sharding import PartitionSpec as P

RESIDUAL_SCALE = 8.0**0.25
NORM_EPSILON = 1e-05
LANES = 128
MESH = pl.DeviceIdType.MESH
F32 = jnp.float32
BF16 = jnp.bfloat16


def layer_norm(values, gain, bias):
    row_mean = jnp.mean(values, axis=-1, keepdims=True)
    spread = jnp.mean(jnp.square(values - row_mean), axis=-1, keepdims=True)
    return (values - row_mean) * lax.rsqrt(spread + NORM_EPSILON) * gain + bias


def expm1_negative(z):
    small = jnp.full_like(z, 1.0 / 40320.0)
    for n in (5040.0, 720.0, 120.0, 24.0, 6.0, 2.0, 1.0):
        small = small * z + 1.0 / n
    return jnp.where(z > -0.5, small * z, jnp.exp(z) - 1.0)


def silu(v):
    return v * jax.nn.sigmoid(v)


def dot(a, b):
    return jnp.dot(a, b, preferred_element_type=F32)


def kernel(
    dims,
    stream, rec_in, gate_in, taps, gates, rate, extra, n1g, n1b, n2g, n2b, wdense,
    out_w_hbm, rg_hbm, ru_hbm, rd_hbm, sg_hbm, su_hbm, sd_hbm,
    result,
    padded, halo, carry_own, carry_in, w_own, w_in, out_w, w_gu, w_d, s_gu, s_d,
    part, part_in, rows, hid, y_part, x_in, z_out, z_in, moe,
    local_sem, halo_sem, carry_send, carry_recv, w_send, w_recv,
    wt_send, wt_recv, tp_send, tp_recv, ag_send, ag_recv, fw_send, fw_recv,
    xs_send, xs_recv, zs_send, zs_recv,
):
    sp_n, tp_n, inner = dims
    outer = sp_n // inner
    pairs = tp_n // 2
    sp, tp = lax.axis_index("sp"), lax.axis_index("tp")
    zi, xi = sp // inner, lax.rem(sp, inner)
    other_x = lax.rem(xi + 1, inner)
    x_peer = zi * inner + other_x
    half_c = lax.rem(tp, 2)
    yi = tp // 2
    mate = yi * 2 + (1 - half_c)
    length, chans = rec_in.shape
    quarter = stream.shape[0]
    fe = rg_hbm.shape[1]
    fs = sg_hbm.shape[1]

    def remote(src, dst, send, recv, where):
        return pltpu.make_async_remote_copy(
            src_ref=src, dst_ref=dst, send_sem=send, recv_sem=recv,
            device_id=where, device_id_type=MESH,
        )

    locals_ = [
        pltpu.make_async_copy(rg_hbm, w_gu.at[tp, :, pl.ds(0, fe)], local_sem.at[0]),
        pltpu.make_async_copy(ru_hbm, w_gu.at[tp, :, pl.ds(fe, fe)], local_sem.at[1]),
        pltpu.make_async_copy(rd_hbm, w_d.at[tp], local_sem.at[2]),
        pltpu.make_async_copy(out_w_hbm, out_w, local_sem.at[3]),
        pltpu.make_async_copy(sg_hbm, s_gu.at[:, pl.ds(0, fs)], local_sem.at[4]),
        pltpu.make_async_copy(su_hbm, s_gu.at[:, pl.ds(fs, fs)], local_sem.at[5]),
        pltpu.make_async_copy(sd_hbm, s_d, local_sem.at[6]),
    ]

    halo_copy = remote(
        rec_in.at[pl.ds(length - 16, 16)], halo, halo_sem.at[0], halo_sem.at[1],
        (lax.rem(sp + 1, sp_n), tp),
    )
    halo_copy.start()

    def weight_dst(slot, kind):
        if kind == 0:
            return w_gu.at[slot, :, pl.ds(0, fe)]
        if kind == 1:
            return w_gu.at[slot, :, pl.ds(fe, fe)]
        return w_d.at[slot]

    sources = (rg_hbm, ru_hbm, rd_hbm)

    def weight_out(kind, step):
        return remote(
            sources[kind], weight_dst(tp, kind),
            wt_send.at[kind, step], wt_recv.at[kind, tp],
            (sp, lax.rem(yi + step, pairs) * 2 + half_c),
        )

    def weight_mate(kind, slot, step):
        src = sources[kind] if step == 0 else weight_dst(slot, kind)
        return remote(
            src, weight_dst(slot, kind),
            wt_send.at[kind, pairs + step], wt_recv.at[kind, slot], (sp, mate),
        )

    def pair_slot(step):
        return lax.rem(yi + step, pairs) * 2 + half_c

    for kind in range(3):
        for step in range(1, pairs):
            weight_out(kind, step).start()
    locals_[3].start()
    for kind in range(3):
        weight_mate(kind, tp, 0).start()
        locals_[kind].start()
    for i in (4, 5, 6):
        locals_[i].start()

    w_own_copy = pltpu.make_async_copy(wdense, w_in.at[sp], local_sem.at[7])
    w_own_copy.start()

    def w_out(step):
        return remote(
            wdense, w_in.at[sp], w_send.at[step], w_recv.at[sp], (lax.rem(sp + step, sp_n), tp)
        )

    @pl.loop(1, sp_n)
    def _(step):
        w_out(step).start()

    padded[pl.ds(8, length)] = rec_in[...].astype(F32)
    halo_copy.wait()
    border = halo[...].astype(F32)[8:16]
    padded[pl.ds(0, 8)] = jnp.where(sp > 0, border, jnp.zeros_like(border))
    tap_n = taps.shape[0]
    summed = taps[0:1] * padded[pl.ds(8 - tap_n + 1, length)]
    for k in range(1, tap_n):
        summed = summed + taps[k : k + 1] * padded[pl.ds(8 - tap_n + 1 + k, length)]
    conv = summed.astype(BF16)
    half = chans // 2
    first = dot(conv[:, :half], gates[0])
    second = dot(conv[:, half:], gates[1])
    recur = jax.nn.sigmoid(jnp.concatenate([first[:, :half], second[:, :half]], axis=1))
    inp = jax.nn.sigmoid(jnp.concatenate([first[:, half:], second[:, half:]], axis=1))
    log_decay = recur * rate[...] + extra[...]
    decay = jnp.exp(log_decay)
    state = jnp.sqrt(-expm1_negative(2.0 * log_decay)) * inp * conv.astype(F32)
    row_id = lax.broadcasted_iota(jnp.int32, (length, chans), 0)
    shift = 1
    while shift < length:
        live = row_id >= shift
        before_a = jnp.where(live, pltpu.roll(decay, shift, 0), 1.0)
        before_b = jnp.where(live, pltpu.roll(state, shift, 0), 0.0)
        state = decay * before_b + state
        decay = decay * before_a
        shift *= 2
    carry_own[...] = jnp.concatenate(
        [decay[length - 1 :], state[length - 1 :], jnp.zeros((6, chans), F32)], axis=0
    )

    def carry_out(step):
        return remote(
            carry_own, carry_in.at[sp], carry_send.at[step], carry_recv.at[sp],
            (lax.rem(sp + step, sp_n), tp),
        )

    def carry_arrival(who):
        return remote(
            carry_own, carry_in.at[who], carry_send.at[0], carry_recv.at[who], (sp, tp)
        )

    @pl.loop(1, sp_n)
    def _(step):
        carry_out(step).start()

    gi = gate_in[...].astype(F32)
    gelu = 0.5 * gi * (1.0 + jnp.tanh(0.7978845608028654 * (gi + 0.044715 * gi * gi * gi)))

    @pl.loop(1, sp_n)
    def _(step):
        carry_arrival(lax.rem(sp + step, sp_n)).wait_recv()

    carry_in[sp] = carry_own[...]

    def fold(who, incoming):
        link = carry_in[who]
        return jnp.where(who < sp, link[0:1] * incoming + link[1:2], incoming)

    incoming = lax.fori_loop(0, sp_n, fold, jnp.zeros((1, chans), F32))
    branch = (gelu * (state + decay * incoming)).astype(BF16)
    locals_[3].wait()
    part[...] = dot(branch, out_w[...]).astype(BF16).reshape(part.shape)

    def part_out(step):
        to = lax.rem(tp + step, tp_n)
        return remote(
            part.at[to], part_in.at[tp], tp_send.at[step], tp_recv.at[tp], (sp, to)
        )

    def part_arrival(who):
        return remote(part.at[who], part_in.at[who], tp_send.at[0], tp_recv.at[who], (sp, tp))

    for step in range(1, tp_n):
        part_out(step).start()
    mixed = part[tp].astype(F32)
    for step in range(1, tp_n):
        who = lax.rem(tp + step, tp_n)
        part_arrival(who).wait_recv()
        mixed = mixed + part_in[who].astype(F32)
    normed = layer_norm(
        RESIDUAL_SCALE * stream[...].astype(F32) + mixed, n1g[...], n1b[...]
    ).astype(BF16)
    rows[sp] = normed

    def ag_out(step):
        return remote(
            rows.at[sp], rows.at[sp], ag_send.at[step], ag_recv.at[sp],
            (lax.rem(zi + step, outer) * inner + xi, tp),
        )

    def ag_arrival(who):
        return remote(rows.at[who], rows.at[who], ag_send.at[0], ag_recv.at[who], (sp, tp))

    def forward(who):
        return remote(
            rows.at[who], rows.at[who], fw_send.at[who], ag_recv.at[who], (x_peer, tp)
        )

    @pl.loop(1, outer)
    def _(step):
        ag_out(step).start()

    forward(sp).start()

    def weight_arrival(kind, slot):
        return remote(
            weight_dst(slot, kind), weight_dst(slot, kind),
            wt_send.at[kind, 0], wt_recv.at[kind, slot], (sp, mate),
        )

    locals_[4].wait()
    locals_[5].wait()
    locals_[6].wait()
    up = dot(normed, s_gu[...])
    s_hid = (silu(up[:, :fs]) * up[:, fs:]).astype(BF16)
    moe[...] = dot(s_hid, s_d[...]) + RESIDUAL_SCALE * normed.astype(F32)

    @pl.loop(1, sp_n)
    def _(step):
        who = lax.rem(sp + step, sp_n)
        remote(wdense, w_in.at[who], w_send.at[0], w_recv.at[who], (sp, tp)).wait_recv()

    w_own_copy.wait()
    for kind in range(3):
        for step in range(1, pairs):
            weight_arrival(kind, pair_slot(step)).wait_recv()
            weight_mate(kind, pair_slot(step), step).start()
    for kind in range(3):
        locals_[kind].wait()
        for step in range(pairs):
            weight_arrival(kind, lax.rem(yi + step, pairs) * 2 + 1 - half_c).wait_recv()

    width = stream.shape[1]
    grp = inner * quarter

    def x_out(zj):
        return remote(
            y_part.at[zj * inner + other_x], x_in.at[zj], xs_send.at[zj], xs_recv.at[zj],
            (x_peer, tp),
        )

    @pl.loop(0, outer)
    def _(step):
        zj = lax.rem(zi + step, outer)
        mine, theirs = zj * inner + xi, zj * inner + other_x

        @pl.when(step > 0)
        def _():
            ag_arrival(mine).wait_recv()
            forward(mine).start()

        ag_arrival(theirs).wait_recv()
        block = rows[pl.ds(zj * inner, inner)].reshape(grp, width)
        for t in range(tp_n):
            gu = dot(block, w_gu[t])
            hid[:, t * fe : (t + 1) * fe] = (silu(gu[:, :fe]) * gu[:, fe:]).astype(BF16)
        wv = w_in[pl.ds(zj * inner, inner)].reshape(grp, w_in.shape[2])
        lane = lax.broadcasted_iota(jnp.int32, wv.shape, 1)
        weight = jnp.sum(jnp.where(lane == sp, wv, 0.0), axis=1, keepdims=True)
        value = weight * dot(hid[...], w_d[...].reshape(tp_n * fe, width))
        y_part[pl.ds(zj * inner, inner)] = value.astype(BF16).reshape(inner, quarter, width)
        x_out(zj).start()

    def z_send(step):
        zj = lax.rem(zi + step, outer)
        return remote(
            z_out.at[zj], z_in.at[zi], zs_send.at[step], zs_recv.at[zi], (zj * inner + xi, tp)
        )

    @pl.loop(1, outer)
    def _(step):
        zj = lax.rem(zi + step, outer)
        x_out(zj).wait_recv()
        both = y_part[zj * inner + xi].astype(F32) + x_in[zj].astype(F32)
        z_out[zj] = both.astype(BF16)
        z_send(step).start()

    x_out(zi).wait_recv()
    moe[...] += y_part[sp].astype(F32) + x_in[zi].astype(F32)

    @pl.loop(1, outer)
    def _(step):
        zj = lax.rem(zi + step, outer)
        remote(z_out.at[zj], z_in.at[zj], zs_send.at[0], zs_recv.at[zj], (sp, tp)).wait_recv()
        moe[...] += z_in[zj].astype(F32)

    result[...] = layer_norm(moe[...], n2g[...], n2b[...]).astype(BF16)

    for kind in range(3):
        for step in range(1, pairs):
            weight_out(kind, step).wait_send()
            weight_mate(kind, pair_slot(step), step).wait_send()
        weight_mate(kind, tp, 0).wait_send()
    for step in range(1, tp_n):
        part_out(step).wait_send()

    @pl.loop(1, sp_n)
    def _(step):
        w_out(step).wait_send()
        carry_out(step).wait_send()

    @pl.loop(1, outer)
    def _(step):
        ag_out(step).wait_send()
        z_send(step).wait_send()

    @pl.loop(0, outer)
    def _(step):
        forward(step * inner + xi).wait_send()
        x_out(step).wait_send()


def block_diagonal(maps):
    kinds, heads, size, _ = maps.shape
    eye = jnp.eye(heads, dtype=maps.dtype)
    spread = maps[:, :, :, None, :] * eye[None, :, None, :, None]
    spread = spread.reshape(kinds, heads * size, heads * size)
    return jnp.concatenate([spread[i] for i in range(kinds)], axis=1)


def shards(
    dims,
    stream,
    recurrence_input,
    output_gate_input,
    convolution_taps,
    first_group_gates,
    second_group_gates,
    channel_decay,
    position_log_extra,
    recurrence_output_weight,
    first_norm_gain,
    first_norm_bias,
    routed_expert_index,
    routed_expert_weight,
    routed_gate_weight,
    routed_up_weight,
    routed_down_weight,
    shared_gate_weight,
    shared_up_weight,
    shared_down_weight,
    second_norm_gain,
    second_norm_bias,
):
    sp_n, tp_n, inner = dims
    outer = sp_n // inner
    length = recurrence_input.shape[0]
    chans = 2 * recurrence_input.shape[2]
    quarter, width = stream.shape
    fe = routed_gate_weight.shape[2]
    fs = shared_gate_weight.shape[1]
    lanes = -(-sp_n // LANES) * LANES
    flat = lambda a: a.reshape(a.shape[0], chans)
    gates = jnp.stack([block_diagonal(first_group_gates), block_diagonal(second_group_gates)])
    rate = (-8.0 * jax.nn.softplus(-channel_decay)).reshape(1, chans)
    own = lax.axis_index("tp") * quarter
    ids = lax.dynamic_slice_in_dim(routed_expert_index, own, quarter, 0)
    wts = lax.dynamic_slice_in_dim(routed_expert_weight, own, quarter, 0)
    hits = ids[:, :, None] == jnp.arange(lanes, dtype=jnp.int32)[None, None, :]
    wdense = jnp.sum(jnp.where(hits, wts[:, :, None], 0.0), axis=1)
    vec = lambda a: a.reshape(1, width)
    vmem = pl.BlockSpec(memory_space=pltpu.VMEM)
    hbm = pl.BlockSpec(memory_space=pl.ANY)
    dma = pltpu.SemaphoreType.DMA
    block = (quarter, width)
    pairs = tp_n // 2
    return pl.pallas_call(
        functools.partial(kernel, dims),
        out_shape=jax.ShapeDtypeStruct(block, BF16),
        in_specs=[vmem] * 12 + [hbm] * 7,
        out_specs=vmem,
        scratch_shapes=[
            pltpu.VMEM((length + 8, chans), F32),
            pltpu.VMEM((16, chans), BF16),
            pltpu.VMEM((8, chans), F32),
            pltpu.VMEM((sp_n, 8, chans), F32),
            pltpu.VMEM((8, LANES), F32),
            pltpu.VMEM((sp_n, quarter, lanes), F32),
            pltpu.VMEM((chans, width), BF16),
            pltpu.VMEM((tp_n, width, 2 * fe), BF16),
            pltpu.VMEM((tp_n, fe, width), BF16),
            pltpu.VMEM((width, 2 * fs), BF16),
            pltpu.VMEM((fs, width), BF16),
            pltpu.VMEM((tp_n,) + block, BF16),
            pltpu.VMEM((tp_n,) + block, BF16),
            pltpu.VMEM((sp_n,) + block, BF16),
            pltpu.VMEM((inner * quarter, tp_n * fe), BF16),
            pltpu.VMEM((sp_n,) + block, BF16),
            pltpu.VMEM((outer,) + block, BF16),
            pltpu.VMEM((outer,) + block, BF16),
            pltpu.VMEM((outer,) + block, BF16),
            pltpu.VMEM(block, F32),
            dma((8,)),
            dma((2,)),
            dma((sp_n,)),
            dma((sp_n,)),
            dma((sp_n,)),
            dma((sp_n,)),
            dma((3, 2 * pairs)),
            dma((3, tp_n)),
            dma((tp_n,)),
            dma((tp_n,)),
            dma((outer,)),
            dma((sp_n,)),
            dma((sp_n,)),
            dma((1,)),
            dma((outer,)),
            dma((outer,)),
            dma((outer,)),
            dma((outer,)),
        ],
        compiler_params=pltpu.CompilerParams(
            has_side_effects=True, vmem_limit_bytes=60 * 2**20
        ),
    )(
        stream,
        flat(recurrence_input),
        flat(output_gate_input),
        flat(convolution_taps).astype(F32),
        gates,
        rate,
        flat(position_log_extra),
        vec(first_norm_gain),
        vec(first_norm_bias),
        vec(second_norm_gain),
        vec(second_norm_bias),
        wdense,
        recurrence_output_weight.reshape(chans, width),
        routed_gate_weight.reshape(width, fe),
        routed_up_weight.reshape(width, fe),
        routed_down_weight.reshape(fe, width),
        shared_gate_weight,
        shared_up_weight,
        shared_down_weight,
    )


def solution(mesh):
    in_specs = (
        P(("sp", "tp"), None),
        P("sp", None, "tp"),
        P("sp", None, "tp"),
        P(None, None, "tp"),
        P(None, "tp", None, None),
        P(None, "tp", None, None),
        P(None, "tp"),
        P("sp", None, "tp"),
        P(None, "tp", None),
        P(),
        P(),
        P("sp", None),
        P("sp", None),
        P("sp", None, "tp"),
        P("sp", None, "tp"),
        P("sp", "tp", None),
        P(),
        P(),
        P(),
        P(),
        P(),
    )
    dims = (mesh.shape["sp"], mesh.shape["tp"], 2)
    return jax.shard_map(
        functools.partial(shards, dims),
        mesh=mesh,
        in_specs=in_specs,
        out_specs=P(("sp", "tp"), None),
        check_vma=False,
    )
```

```python
import functools

import jax
import jax.numpy as jnp
from jax import lax
from jax.experimental import pallas as pl
from jax.experimental.pallas import tpu as pltpu
from jax.sharding import PartitionSpec as P

RESIDUAL_SCALE = 8.0**0.25
NORM_EPSILON = 1e-05
LANES = 128
PIECES = 6
EARLY = 3
MESH = pl.DeviceIdType.MESH
F32 = jnp.float32
BF16 = jnp.bfloat16


def layer_norm(values, gain, bias):
    row_mean = jnp.mean(values, axis=-1, keepdims=True)
    spread = jnp.mean(jnp.square(values - row_mean), axis=-1, keepdims=True)
    return (values - row_mean) * lax.rsqrt(spread + NORM_EPSILON) * gain + bias


def expm1_negative(z):
    small = jnp.full_like(z, 1.0 / 40320.0)
    for n in (5040.0, 720.0, 120.0, 24.0, 6.0, 2.0, 1.0):
        small = small * z + 1.0 / n
    return jnp.where(z > -0.5, small * z, jnp.exp(z) - 1.0)


def softplus(y):
    u = jnp.exp(-jnp.abs(y))
    s = u / (2.0 + u)
    sq = s * s
    series = jnp.full_like(s, 1.0 / 17.0)
    for n in (15.0, 13.0, 11.0, 9.0, 7.0, 5.0, 3.0, 1.0):
        series = series * sq + 1.0 / n
    return jnp.maximum(y, 0.0) + 2.0 * s * series


def lane_blocks(maps_ref):
    kinds, heads, size, _ = maps_ref.shape
    per = LANES // size
    blocks = []
    for start in range(0, heads, per):
        sides = []
        for kind in range(kinds):
            if per == 1:
                sides.append(maps_ref[kind, start])
                continue
            tall = []
            for p in range(per):
                row = lax.broadcasted_iota(jnp.int32, (size, LANES), 0)
                col = lax.broadcasted_iota(jnp.int32, (size, LANES), 1)
                place = jnp.where(col == row + p * size, 1.0, 0.0).astype(BF16)
                tall.append(dot(maps_ref[kind, start + p], place))
            sides.append(jnp.concatenate(tall, axis=0).astype(BF16))
        blocks.append(jnp.concatenate(sides, axis=1))
    return blocks


def silu(v):
    return v * jax.nn.sigmoid(v)


def dot(a, b):
    return jnp.dot(a, b, preferred_element_type=F32)


def kernel(
    dims,
    stream, rec_in, gate_in, taps, small_maps, large_maps, channel_decay, extra, n1g, n1b, n2g, n2b,
    ids, wts,
    out_w_hbm, rg_hbm, ru_hbm, rd_hbm, sg_hbm, su_hbm, sd_hbm,
    result,
    padded, halo, carry_own, carry_in, wdense, w_in, out_w, w_gu, w_d, s_gu, s_d,
    part, part_in, rows, hid, y_part, x_in, z_out, z_in, moe,
    local_sem, halo_sem, carry_send, carry_recv, w_send, w_recv,
    wt_send, wt_recv, tp_send, tp_recv, ag_send, ag_recv, fw_send, fw_recv,
    xs_send, xs_recv, zs_send, zs_recv,
):
    sp_n, tp_n, inner = dims
    outer = sp_n // inner
    pairs = tp_n // 2
    sp, tp = lax.axis_index("sp"), lax.axis_index("tp")
    zi, xi = sp // inner, lax.rem(sp, inner)
    other_x = lax.rem(xi + 1, inner)
    x_peer = zi * inner + other_x
    half_c = lax.rem(tp, 2)
    yi = tp // 2
    mate = yi * 2 + (1 - half_c)
    length, chans = rec_in.shape
    quarter = stream.shape[0]
    fe = rg_hbm.shape[1]
    fs = sg_hbm.shape[1]

    def remote(src, dst, send, recv, where):
        return pltpu.make_async_remote_copy(
            src_ref=src, dst_ref=dst, send_sem=send, recv_sem=recv,
            device_id=where, device_id_type=MESH,
        )

    locals_ = [
        pltpu.make_async_copy(rg_hbm, w_gu.at[tp, :, pl.ds(0, fe)], local_sem.at[0]),
        pltpu.make_async_copy(ru_hbm, w_gu.at[tp, :, pl.ds(fe, fe)], local_sem.at[1]),
        pltpu.make_async_copy(rd_hbm, w_d.at[tp], local_sem.at[2]),
        pltpu.make_async_copy(out_w_hbm, out_w, local_sem.at[3]),
        pltpu.make_async_copy(sg_hbm, s_gu.at[:, pl.ds(0, fs)], local_sem.at[4]),
        pltpu.make_async_copy(su_hbm, s_gu.at[:, pl.ds(fs, fs)], local_sem.at[5]),
        pltpu.make_async_copy(sd_hbm, s_d, local_sem.at[6]),
    ]

    halo_copy = remote(
        rec_in.at[pl.ds(length - 16, 16)], halo, halo_sem.at[0], halo_sem.at[1],
        (lax.rem(sp + 1, sp_n), tp),
    )
    halo_copy.start()

    depth = rg_hbm.shape[0] // 2
    fe_half = fe // 2

    def weight_src(piece):
        kind, part_id = piece // 2, piece % 2
        if kind == 2:
            return rd_hbm.at[pl.ds(part_id * fe_half, fe_half)]
        return (rg_hbm, ru_hbm)[kind].at[pl.ds(part_id * depth, depth)]

    def weight_dst(slot, piece):
        kind, part_id = piece // 2, piece % 2
        if kind == 2:
            return w_d.at[slot, pl.ds(part_id * fe_half, fe_half)]
        return w_gu.at[slot, pl.ds(part_id * depth, depth), pl.ds(kind * fe, fe)]

    def weight_out(kind, step):
        return remote(
            weight_src(kind), weight_dst(tp, kind),
            wt_send.at[kind, step], wt_recv.at[kind, tp],
            (sp, lax.rem(yi + step, pairs) * 2 + half_c),
        )

    def weight_mate(kind, slot, step):
        src = weight_src(kind) if step == 0 else weight_dst(slot, kind)
        return remote(
            src, weight_dst(slot, kind),
            wt_send.at[kind, pairs + step], wt_recv.at[kind, slot], (sp, mate),
        )

    def pair_slot(step):
        return lax.rem(yi + step, pairs) * 2 + half_c

    for piece in range(EARLY):
        for step in range(1, pairs):
            weight_out(piece, step).start()
    locals_[3].start()
    for piece in range(PIECES):
        weight_mate(piece, tp, 0).start()
    for i in range(3):
        locals_[i].start()
    for i in (4, 5, 6):
        locals_[i].start()

    expert = lax.broadcasted_iota(jnp.int32, (wdense.shape[0], length), 0)
    table = jnp.zeros((wdense.shape[0], length), F32)
    for k in range(ids.shape[0]):
        table = table + jnp.where(expert == ids[k : k + 1], wts[k : k + 1], 0.0)
    wdense[...] = table
    w_in[sp] = table

    def w_out(step):
        return remote(
            wdense, w_in.at[sp], w_send.at[step], w_recv.at[sp], (lax.rem(sp + step, sp_n), tp)
        )

    @pl.loop(1, sp_n)
    def _(step):
        w_out(step).start()

    small_blocks, large_blocks = lane_blocks(small_maps), lane_blocks(large_maps)
    rate_rows = -8.0 * softplus(-channel_decay[...])
    rate = jnp.concatenate([rate_rows[0:1], rate_rows[1:2]], axis=1)
    tap_rows = [
        jnp.concatenate([taps[k, 0:1], taps[k, 1:2]], axis=1).astype(F32)
        for k in range(taps.shape[0])
    ]

    padded[pl.ds(8, length)] = rec_in[...].astype(F32)
    halo_copy.wait()
    border = halo[...].astype(F32)[8:16]
    padded[pl.ds(0, 8)] = jnp.where(sp > 0, border, jnp.zeros_like(border))
    tap_n = taps.shape[0]
    summed = tap_rows[0] * padded[pl.ds(8 - tap_n + 1, length)]
    for k in range(1, tap_n):
        summed = summed + tap_rows[k] * padded[pl.ds(8 - tap_n + 1 + k, length)]
    conv = summed.astype(BF16)
    outs = [
        dot(conv[:, i * LANES : (i + 1) * LANES], maps)
        for i, maps in enumerate(small_blocks + large_blocks)
    ]
    recur = jax.nn.sigmoid(jnp.concatenate([o[:, :LANES] for o in outs], axis=1))
    inp = jax.nn.sigmoid(jnp.concatenate([o[:, LANES:] for o in outs], axis=1))
    log_decay = recur * rate + extra[...]
    decay = jnp.exp(log_decay)
    state = jnp.sqrt(-expm1_negative(2.0 * log_decay)) * inp * conv.astype(F32)
    row_id = lax.broadcasted_iota(jnp.int32, (length, chans), 0)
    shift = 1
    while shift < length:
        live = row_id >= shift
        before_a = jnp.where(live, pltpu.roll(decay, shift, 0), 1.0)
        before_b = jnp.where(live, pltpu.roll(state, shift, 0), 0.0)
        state = decay * before_b + state
        decay = decay * before_a
        shift *= 2
    carry_own[...] = jnp.concatenate(
        [decay[length - 1 :], state[length - 1 :], jnp.zeros((6, chans), F32)], axis=0
    )

    def carry_out(step):
        return remote(
            carry_own, carry_in.at[sp], carry_send.at[step], carry_recv.at[sp],
            (lax.rem(sp + step, sp_n), tp),
        )

    def carry_arrival(who):
        return remote(
            carry_own, carry_in.at[who], carry_send.at[0], carry_recv.at[who], (sp, tp)
        )

    @pl.loop(1, sp_n)
    def _(step):
        carry_out(step).start()

    gi = gate_in[...].astype(F32)
    gelu = 0.5 * gi * (1.0 + jnp.tanh(0.7978845608028654 * (gi + 0.044715 * gi * gi * gi)))

    @pl.loop(1, sp_n)
    def _(step):
        carry_arrival(lax.rem(sp + step, sp_n)).wait_recv()

    carry_in[sp] = carry_own[...]

    def fold(who, incoming):
        link = carry_in[who]
        return jnp.where(who < sp, link[0:1] * incoming + link[1:2], incoming)

    incoming = lax.fori_loop(0, sp_n, fold, jnp.zeros((1, chans), F32))
    branch = (gelu * (state + decay * incoming)).astype(BF16)
    locals_[3].wait()
    part[...] = dot(branch, out_w[...]).astype(BF16).reshape(part.shape)

    def part_out(step):
        to = lax.rem(tp + step, tp_n)
        return remote(
            part.at[to], part_in.at[tp], tp_send.at[step], tp_recv.at[tp], (sp, to)
        )

    def part_arrival(who):
        return remote(part.at[who], part_in.at[who], tp_send.at[0], tp_recv.at[who], (sp, tp))

    for step in range(1, tp_n):
        part_out(step).start()
    for piece in range(EARLY, PIECES):
        for step in range(1, pairs):
            weight_out(piece, step).start()
    mixed = part[tp].astype(F32)
    for step in range(1, tp_n):
        who = lax.rem(tp + step, tp_n)
        part_arrival(who).wait_recv()
        mixed = mixed + part_in[who].astype(F32)
    normed = layer_norm(
        RESIDUAL_SCALE * stream[...].astype(F32) + mixed, n1g[...], n1b[...]
    ).astype(BF16)
    rows[sp] = normed

    def ag_out(step):
        return remote(
            rows.at[sp], rows.at[sp], ag_send.at[step], ag_recv.at[sp],
            (lax.rem(zi + step, outer) * inner + xi, tp),
        )

    def ag_arrival(who):
        return remote(rows.at[who], rows.at[who], ag_send.at[0], ag_recv.at[who], (sp, tp))

    def forward(who):
        return remote(
            rows.at[who], rows.at[who], fw_send.at[who], ag_recv.at[who], (x_peer, tp)
        )

    @pl.loop(1, outer)
    def _(step):
        ag_out(step).start()

    forward(sp).start()

    def weight_arrival(kind, slot):
        return remote(
            weight_dst(slot, kind), weight_dst(slot, kind),
            wt_send.at[kind, 0], wt_recv.at[kind, slot], (sp, mate),
        )

    def relay(piece):
        for step in range(1, pairs):
            weight_arrival(piece, pair_slot(step)).wait_recv()
            weight_mate(piece, pair_slot(step), step).start()

    for piece in range(EARLY):
        relay(piece)

    locals_[4].wait()
    locals_[5].wait()
    locals_[6].wait()
    up = dot(normed, s_gu[...])
    s_hid = (silu(up[:, :fs]) * up[:, fs:]).astype(BF16)
    moe[...] = dot(s_hid, s_d[...]) + RESIDUAL_SCALE * normed.astype(F32)

    @pl.loop(1, sp_n)
    def _(step):
        who = lax.rem(sp + step, sp_n)
        remote(wdense, w_in.at[who], w_send.at[0], w_recv.at[who], (sp, tp)).wait_recv()

    for i in range(3):
        locals_[i].wait()

    @pl.loop(1, outer)
    def _(step):
        mine = lax.rem(zi + step, outer) * inner + xi
        ag_arrival(mine).wait_recv()
        forward(mine).start()

    for piece in range(EARLY, PIECES):
        relay(piece)

    @pl.loop(0, outer)
    def _(step):
        ag_arrival(step * inner + other_x).wait_recv()

    for piece in range(PIECES):
        for step in range(pairs):
            weight_arrival(piece, lax.rem(yi + step, pairs) * 2 + 1 - half_c).wait_recv()

    width = stream.shape[1]
    grp = inner * quarter
    batch = min(sp_n, 8)

    @pl.loop(0, sp_n // batch)
    def _(i):
        block = rows[pl.ds(i * batch, batch)].reshape(batch * quarter, width)
        for t in range(tp_n):
            gu = dot(block, w_gu[t])
            act = (silu(gu[:, :fe]) * gu[:, fe:]).astype(BF16)
            hid[pl.ds(i * batch, batch), :, t * fe : (t + 1) * fe] = act.reshape(
                batch, quarter, fe
            )

    def x_out(zj):
        return remote(
            y_part.at[zj * inner + other_x], x_in.at[zj], xs_send.at[zj], xs_recv.at[zj],
            (x_peer, tp),
        )

    own_rows = lax.broadcasted_iota(jnp.int32, (quarter, length), 0) + tp * quarter
    pick = lax.broadcasted_iota(jnp.int32, (quarter, length), 1) == own_rows

    @pl.loop(1, outer + 1)
    def _(step):
        zj = lax.rem(zi + step, outer)
        block = hid[pl.ds(zj * inner, inner)].reshape(grp, tp_n * fe)
        value = dot(block, w_d[...].reshape(tp_n * fe, width))
        for j in range(inner):
            line = w_in[zj * inner + j, pl.ds(sp, 1)]
            weight = jnp.sum(jnp.where(pick, line, 0.0), axis=1, keepdims=True)
            y_part[zj * inner + j] = (
                weight * value[j * quarter : (j + 1) * quarter]
            ).astype(BF16)
        x_out(zj).start()

    def z_send(step):
        zj = lax.rem(zi + step, outer)
        return remote(
            z_out.at[zj], z_in.at[zi], zs_send.at[step], zs_recv.at[zi], (zj * inner + xi, tp)
        )

    @pl.loop(1, outer)
    def _(step):
        zj = lax.rem(zi + step, outer)
        x_out(zj).wait_recv()
        both = y_part[zj * inner + xi].astype(F32) + x_in[zj].astype(F32)
        z_out[zj] = both.astype(BF16)
        z_send(step).start()

    x_out(zi).wait_recv()
    moe[...] += y_part[sp].astype(F32) + x_in[zi].astype(F32)

    @pl.loop(1, outer)
    def _(step):
        zj = lax.rem(zi + step, outer)
        remote(z_out.at[zj], z_in.at[zj], zs_send.at[0], zs_recv.at[zj], (sp, tp)).wait_recv()
        moe[...] += z_in[zj].astype(F32)

    result[...] = layer_norm(moe[...], n2g[...], n2b[...]).astype(BF16)

    for kind in range(PIECES):
        for step in range(1, pairs):
            weight_out(kind, step).wait_send()
            weight_mate(kind, pair_slot(step), step).wait_send()
        weight_mate(kind, tp, 0).wait_send()
    for step in range(1, tp_n):
        part_out(step).wait_send()

    @pl.loop(1, sp_n)
    def _(step):
        w_out(step).wait_send()
        carry_out(step).wait_send()

    @pl.loop(1, outer)
    def _(step):
        ag_out(step).wait_send()
        z_send(step).wait_send()

    @pl.loop(0, outer)
    def _(step):
        forward(step * inner + xi).wait_send()
        x_out(step).wait_send()


def shards(
    dims,
    stream,
    recurrence_input,
    output_gate_input,
    convolution_taps,
    first_group_gates,
    second_group_gates,
    channel_decay,
    position_log_extra,
    recurrence_output_weight,
    first_norm_gain,
    first_norm_bias,
    routed_expert_index,
    routed_expert_weight,
    routed_gate_weight,
    routed_up_weight,
    routed_down_weight,
    shared_gate_weight,
    shared_up_weight,
    shared_down_weight,
    second_norm_gain,
    second_norm_bias,
):
    sp_n, tp_n, inner = dims
    outer = sp_n // inner
    length = recurrence_input.shape[0]
    chans = 2 * recurrence_input.shape[2]
    quarter, width = stream.shape
    fe = routed_gate_weight.shape[2]
    fs = shared_gate_weight.shape[1]
    flat = lambda a: a.reshape(a.shape[0], chans)
    vec = lambda a: a.reshape(1, width)
    vmem = pl.BlockSpec(memory_space=pltpu.VMEM)
    hbm = pl.BlockSpec(memory_space=pl.ANY)
    dma = pltpu.SemaphoreType.DMA
    block = (quarter, width)
    pairs = tp_n // 2
    return pl.pallas_call(
        functools.partial(kernel, dims),
        out_shape=jax.ShapeDtypeStruct(block, BF16),
        in_specs=[vmem] * 14 + [hbm] * 7,
        out_specs=vmem,
        scratch_shapes=[
            pltpu.VMEM((length + 8, chans), F32),
            pltpu.VMEM((16, chans), BF16),
            pltpu.VMEM((8, chans), F32),
            pltpu.VMEM((sp_n, 8, chans), F32),
            pltpu.VMEM((sp_n, length), F32),
            pltpu.VMEM((sp_n, sp_n, length), F32),
            pltpu.VMEM((chans, width), BF16),
            pltpu.VMEM((tp_n, width, 2 * fe), BF16),
            pltpu.VMEM((tp_n, fe, width), BF16),
            pltpu.VMEM((width, 2 * fs), BF16),
            pltpu.VMEM((fs, width), BF16),
            pltpu.VMEM((tp_n,) + block, BF16),
            pltpu.VMEM((tp_n,) + block, BF16),
            pltpu.VMEM((sp_n,) + block, BF16),
            pltpu.VMEM((sp_n, quarter, tp_n * fe), BF16),
            pltpu.VMEM((sp_n,) + block, BF16),
            pltpu.VMEM((outer,) + block, BF16),
            pltpu.VMEM((outer,) + block, BF16),
            pltpu.VMEM((outer,) + block, BF16),
            pltpu.VMEM(block, F32),
            dma((8,)),
            dma((2,)),
            dma((sp_n,)),
            dma((sp_n,)),
            dma((sp_n,)),
            dma((sp_n,)),
            dma((PIECES, 2 * pairs)),
            dma((PIECES, tp_n)),
            dma((tp_n,)),
            dma((tp_n,)),
            dma((outer,)),
            dma((sp_n,)),
            dma((sp_n,)),
            dma((1,)),
            dma((outer,)),
            dma((outer,)),
            dma((outer,)),
            dma((outer,)),
        ],
        compiler_params=pltpu.CompilerParams(
            has_side_effects=True, vmem_limit_bytes=60 * 2**20
        ),
    )(
        stream,
        flat(recurrence_input),
        flat(output_gate_input),
        convolution_taps,
        first_group_gates,
        second_group_gates,
        channel_decay,
        flat(position_log_extra),
        vec(first_norm_gain),
        vec(first_norm_bias),
        vec(second_norm_gain),
        vec(second_norm_bias),
        routed_expert_index.T,
        routed_expert_weight.T,
        recurrence_output_weight.reshape(chans, width),
        routed_gate_weight.reshape(width, fe),
        routed_up_weight.reshape(width, fe),
        routed_down_weight.reshape(fe, width),
        shared_gate_weight,
        shared_up_weight,
        shared_down_weight,
    )


def solution(mesh):
    in_specs = (
        P(("sp", "tp"), None),
        P("sp", None, "tp"),
        P("sp", None, "tp"),
        P(None, None, "tp"),
        P(None, "tp", None, None),
        P(None, "tp", None, None),
        P(None, "tp"),
        P("sp", None, "tp"),
        P(None, "tp", None),
        P(),
        P(),
        P("sp", None),
        P("sp", None),
        P("sp", None, "tp"),
        P("sp", None, "tp"),
        P("sp", "tp", None),
        P(),
        P(),
        P(),
        P(),
        P(),
    )
    dims = (mesh.shape["sp"], mesh.shape["tp"], 2)
    return jax.shard_map(
        functools.partial(shards, dims),
        mesh=mesh,
        in_specs=in_specs,
        out_specs=P(("sp", "tp"), None),
        check_vma=False,
    )
```
